32 devices in a mesh: sp: 8 (over z, x), tp: 4 (over y, core).
Axes of the slice: x: 2, y: 2, z: 4, core: 2. Of those that a mesh axis runs over, the one named last changes fastest.
Arguments:
- tokens: bfloat16 [6144, 4096], P('sp', 'tp'), may hold values from -12 to 12
- query_weight: bfloat16 [4096, 2048], P(None, 'tp'), may hold values from -0.09375 to 0.09375
- key_weight: bfloat16 [4096, 2048], P(None, 'tp'), may hold values from -0.09375 to 0.09375
- value_weight: bfloat16 [4096, 2048], P(None, 'tp'), may hold values from -0.09375 to 0.09375
- position_bias: float32 [16, 320], P('tp'), may hold values from -104 to 154
- out_grad: bfloat16 [6144, 2048], P('sp', 'tp'), may hold values from -6 to 6
Outputs:
- input_grad: bfloat16 [6144, 4096], P('sp', 'tp')
- query_weight_grad: float32 [4096, 2048], P('sp', 'tp')
- key_weight_grad: float32 [4096, 2048], P('sp', 'tp')
- value_weight_grad: float32 [4096, 2048], P('sp', 'tp')
- bias_grad: float32 [16, 320], P('tp')
The draws below stay inside these ranges and needn't reach their ends.
All inputs are finite; a program needn't handle non-finite values.
Results may differ from the reference program's by a relative error of at most 0.014.
Values may be sent and summed in bfloat16 or wider, within the bound.
A program may use at most 128 MiB of HBM per device.

```python
import jax
import jax.numpy as jnp
import numpy as np
from jax import lax

WIDTH = 4096
HEADS = 16
HEAD_DIM = 128
SEGMENT = 64
PREVIOUS = 4
CLIP = 256
TOKENS = 6144
ATT_WIDTH = 2048
BIAS_LEN = 320
N_TP = 4


def draw_tokens(key, part):
    base = jax.random.normal(jax.random.fold_in(key, 11), (TOKENS, WIDTH), jnp.float32)
    base = jnp.clip(base, -6.0, 6.0)
    return base.astype(jnp.bfloat16)


def draw_position_bias(key, part):
    base = jax.random.normal(jax.random.fold_in(key, 21), (HEADS, BIAS_LEN), jnp.float32)
    base = jnp.clip(base, -4.0, 4.0)
    return base.astype(jnp.float32)


def shard_levels(rng, shape, split, smallest, top_value):
    level = 1.0
    for dim, blocks in split:
        heights = jax.random.uniform(jax.random.fold_in(jax.random.fold_in(rng, 6), dim), (blocks,), jnp.float32, smallest / len(split), top_value / len(split))
        level = level * jnp.repeat(jnp.exp(heights), shape[dim] // blocks).reshape((-1,) + (1,) * (len(shape) - 1 - dim))
    return level


def bell_draw(stream_key, extent, scale, most, shards=(), kind=jnp.bfloat16):
    values = scale * jax.random.normal(stream_key, extent, jnp.float32)
    if shards:
        values = values * shard_levels(stream_key, extent, shards, -0.22, 0.18)
    return jnp.clip(values, -most, most).astype(kind)


def setup_inputs(seed: int = 0) -> dict:
    arg_keys = jax.random.split(jax.random.key(seed), 7)
    tokens = draw_tokens(jax.random.fold_in(arg_keys[6], 71), 0)
    query_weight = bell_draw(arg_keys[1], (WIDTH, ATT_WIDTH), WIDTH ** -0.5, 0.09375, ((1, 4),))
    key_weight = bell_draw(arg_keys[2], (WIDTH, ATT_WIDTH), WIDTH ** -0.5, 0.09375, ((1, 4),))
    value_weight = bell_draw(arg_keys[3], (WIDTH, ATT_WIDTH), WIDTH ** -0.5, 0.09375, ((1, 4),))
    position_bias = draw_position_bias(jax.random.fold_in(arg_keys[6], 71), 0)
    out_grad = bell_draw(arg_keys[5], (TOKENS, ATT_WIDTH), 1.0, 6.0, ((0, 8), (1, 4)))
    return {"tokens": tokens, "query_weight": query_weight, "key_weight": key_weight, "value_weight": value_weight, "position_bias": position_bias, "out_grad": out_grad}


def bias_index(segment, reach, clip):
    query_pos = np.arange(segment)[:, None]
    band_pos = np.arange(reach + segment)[None, :]
    return (np.minimum(reach + query_pos - band_pos, clip) + segment - 1).astype(np.int32)


def fold_band(parts, count, head):
    shaped = parts.reshape(count, PREVIOUS + 1, SEGMENT, head)
    total = jnp.zeros((count + PREVIOUS, SEGMENT, head), jnp.float32)
    for band in range(PREVIOUS + 1):
        total = total.at[band:band + count].add(shaped[:, band])
    return total.reshape((count + PREVIOUS) * SEGMENT, head)


def head_grads(operands):
    query, keys, values, upstream, table = operands
    length, head = query.shape
    reach = PREVIOUS * SEGMENT
    count = length // SEGMENT
    factor = head ** -0.5
    padding = jnp.zeros((reach, head), keys.dtype)
    key_seg = jnp.concatenate([padding, keys]).reshape(count + PREVIOUS, SEGMENT, head)
    value_seg = jnp.concatenate([padding, values]).reshape(count + PREVIOUS, SEGMENT, head)
    key_band = jnp.stack([key_seg[band:band + count] for band in range(PREVIOUS + 1)], axis=1).reshape(count, reach + SEGMENT, head)
    value_band = jnp.stack([value_seg[band:band + count] for band in range(PREVIOUS + 1)], axis=1).reshape(count, reach + SEGMENT, head)
    query_seg = query.reshape(count, SEGMENT, head)
    grad_seg = upstream.reshape(count, SEGMENT, head)
    flat_index = bias_index(SEGMENT, reach, CLIP)
    bias = table[flat_index]
    scores = jnp.einsum('cqd,ckd->cqk', query_seg.astype(jnp.float32), key_band.astype(jnp.float32)) * factor + bias[None]
    key_pos = jnp.arange(count)[:, None] * SEGMENT - reach + jnp.arange(reach + SEGMENT)[None, :]
    valid = (key_pos >= 0)[:, None, :]
    masked = jnp.where(valid, scores, -jnp.inf)
    top = jnp.max(masked, axis=-1, keepdims=True)
    logsum = top + jnp.log(jnp.sum(jnp.exp(masked - top), axis=-1, keepdims=True))
    weights = jnp.exp(masked - logsum)
    weights_low = weights.astype(jnp.bfloat16)
    prob_grad = jnp.einsum('cqd,ckd->cqk', grad_seg.astype(jnp.float32), value_band.astype(jnp.float32))
    delta = jnp.sum(weights * prob_grad, axis=-1, keepdims=True)
    score_grad = weights * (prob_grad - delta)
    score_low = score_grad.astype(jnp.bfloat16)
    query_grad = (jnp.einsum('cqk,ckd->cqd', score_low.astype(jnp.float32), key_band.astype(jnp.float32)) * factor).reshape(length, head).astype(jnp.bfloat16)
    key_parts = jnp.einsum('cqk,cqd->ckd', score_low.astype(jnp.float32), query_seg.astype(jnp.float32)) * factor
    value_parts = jnp.einsum('cqk,cqd->ckd', weights_low.astype(jnp.float32), grad_seg.astype(jnp.float32))
    key_grad = fold_band(key_parts, count, head)[reach:].astype(jnp.bfloat16)
    value_grad = fold_band(value_parts, count, head)[reach:].astype(jnp.bfloat16)
    summed = jnp.sum(score_grad, axis=0).reshape(-1)
    table_grad = jnp.zeros((table.shape[0],), jnp.float32).at[flat_index.reshape(-1)].add(summed)
    return query_grad, key_grad, value_grad, table_grad


def reference(tokens, query_weight, key_weight, value_weight, position_bias, out_grad):
    query = jnp.dot(tokens, query_weight, preferred_element_type=jnp.float32).astype(jnp.bfloat16)
    keys = jnp.dot(tokens, key_weight, preferred_element_type=jnp.float32).astype(jnp.bfloat16)
    values = jnp.dot(tokens, value_weight, preferred_element_type=jnp.float32).astype(jnp.bfloat16)

    def by_head(array):
        return array.reshape(TOKENS, HEADS, HEAD_DIM).transpose(1, 0, 2)

    def by_token(array):
        return array.transpose(1, 0, 2).reshape(TOKENS, HEADS * HEAD_DIM)

    head_query, head_key, head_value, bias_grad = lax.map(head_grads, (by_head(query), by_head(keys), by_head(values), by_head(out_grad), position_bias))
    query_grad = by_token(head_query)
    key_grad = by_token(head_key)
    value_grad = by_token(head_value)
    tokens_t = tokens.T
    query_weight_grad = jnp.dot(tokens_t, query_grad, preferred_element_type=jnp.float32)
    key_weight_grad = jnp.dot(tokens_t, key_grad, preferred_element_type=jnp.float32)
    value_weight_grad = jnp.dot(tokens_t, value_grad, preferred_element_type=jnp.float32)
    group = HEADS * HEAD_DIM // N_TP
    total = jnp.zeros((TOKENS, WIDTH), jnp.float32)
    for number in range(N_TP):
        lower = number * group
        upper = lower + group
        term = jnp.dot(query_grad[:, lower:upper], query_weight[:, lower:upper].T, preferred_element_type=jnp.float32)
        term = term + jnp.dot(key_grad[:, lower:upper], key_weight[:, lower:upper].T, preferred_element_type=jnp.float32)
        term = term + jnp.dot(value_grad[:, lower:upper], value_weight[:, lower:upper].T, preferred_element_type=jnp.float32)
        rounded = lax.optimization_barrier(term.astype(jnp.bfloat16))
        total = total + rounded.astype(jnp.float32)
    input_grad = total.astype(jnp.bfloat16)
    return (input_grad, query_weight_grad, key_weight_grad, value_weight_grad, bias_grad)
```

```python
import functools

import jax
import jax.numpy as jnp
from jax import lax
from jax.experimental import pallas as pl
from jax.experimental.pallas import tpu as pltpu
from jax.sharding import PartitionSpec as P

SEGMENT = 64
PREVIOUS = 4
CLIP = 256
ROWS = 2 * SEGMENT
REACH = PREVIOUS * SEGMENT
WINDOW = ROWS + REACH
TABLE = 512
HIDDEN = -1e30


def from_behind(value, axis, steps):
    count = lax.axis_size(axis)
    leading, last = (max(0, -steps), min(count, count - steps))
    return lax.ppermute(value, axis, [(source, source + steps) for source in range(leading, last)])


def contract_rows(left, right):
    return lax.dot_general(
        left, right, (((0,), (0,)), ((), ())), preferred_element_type=jnp.float32
    )


def contract_cols(left, right):
    return lax.dot_general(
        left, right, (((1,), (1,)), ((), ())), preferred_element_type=jnp.float32
    )


def diagonal_sums(tile):
    half = tile.shape[0] // 2
    while half >= 8:
        tile = tile[:half] + pltpu.roll(tile[half:], TABLE - half, 1)
        half //= 2
    row = lax.broadcasted_iota(jnp.int32, tile.shape, 0)
    for step in (4, 2, 1):
        tile = jnp.where((row & step) != 0, pltpu.roll(tile, TABLE - step, 1), tile)
    return jnp.sum(tile, axis=0, keepdims=True)


def attention_kernel(
    factor,
    first_ref,
    q_ref,
    k_ref,
    v_ref,
    pk_ref,
    pv_ref,
    g_ref,
    table_ref,
    dq_ref,
    dk_ref,
    dv_ref,
    dk_tail_ref,
    dv_tail_ref,
    dk_back_ref,
    dv_back_ref,
    table_grad_ref,
    k_all,
    v_all,
    dk_all,
    dv_all,
):
    length = q_ref.shape[0]
    k_all[:REACH] = pk_ref[...]
    k_all[REACH:] = k_ref[...]
    v_all[:REACH] = pv_ref[...]
    v_all[REACH:] = v_ref[...]
    dk_all[...] = jnp.zeros_like(dk_all)
    dv_all[...] = jnp.zeros_like(dv_all)
    first = first_ref[0]
    table = jnp.broadcast_to(table_ref[0], (ROWS, TABLE))
    bias = pltpu.roll(table, 0, 1, stride=1, stride_axis=0)[:, :WINDOW]
    row = lax.broadcasted_iota(jnp.int32, (ROWS, WINDOW), 0) // SEGMENT
    column = lax.broadcasted_iota(jnp.int32, (ROWS, WINDOW), 1)
    behind = column // SEGMENT - row
    bias = jnp.where((behind >= 0) & (behind <= PREVIOUS), bias, HIDDEN)
    bias_sum = jnp.zeros((ROWS, WINDOW), jnp.float32)
    for start in range(0, length, ROWS):
        q = q_ref[start : start + ROWS]
        g = g_ref[start : start + ROWS]
        k = k_all[start : start + WINDOW]
        v = v_all[start : start + WINDOW]
        mask = bias
        if start < REACH:
            mask = jnp.where(column + start < first, HIDDEN, bias)
        scores = contract_cols(q, k) * factor + mask
        top = jnp.max(scores, axis=1, keepdims=True)
        raised = jnp.exp(scores - top)
        weights = raised * (1.0 / jnp.sum(raised, axis=1, keepdims=True))
        prob_grad = contract_cols(g, v)
        delta = jnp.sum(weights * prob_grad, axis=1, keepdims=True)
        score_grad = weights * (prob_grad - delta)
        bias_sum = bias_sum + score_grad
        low = score_grad.astype(jnp.bfloat16)
        dq = jnp.dot(low, k, preferred_element_type=jnp.float32) * factor
        dq_ref[start : start + ROWS] = dq.astype(jnp.bfloat16)
        dk_all[start : start + WINDOW] += contract_rows(low, q)
        dv_all[start : start + WINDOW] += contract_rows(weights.astype(jnp.bfloat16), g)
    dk_back_ref[...] = (dk_all[:REACH] * factor).astype(jnp.bfloat16)
    dv_back_ref[...] = dv_all[:REACH].astype(jnp.bfloat16)
    dk_ref[...] = (dk_all[REACH:length] * factor).astype(jnp.bfloat16)
    dv_ref[...] = dv_all[REACH:length].astype(jnp.bfloat16)
    dk_tail_ref[...] = dk_all[length:] * factor
    dv_tail_ref[...] = dv_all[length:]
    padded = jnp.concatenate([bias_sum, jnp.zeros((ROWS, TABLE - WINDOW), jnp.float32)], axis=1)
    table_grad_ref[0] = diagonal_sums(padded)


def attention(query, keys, values, prev_keys, prev_values, out_grad, position_bias):
    length, width = query.shape
    heads, entries = position_bias.shape
    head = width // heads
    factor = head ** (-0.5)
    table = jnp.concatenate(
        [
            position_bias[:, ::-1],
            jnp.zeros((heads, WINDOW - entries), jnp.float32),
            jnp.broadcast_to(position_bias[:, entries - 1 :], (heads, TABLE - WINDOW)),
        ],
        axis=1,
    )[:, None]
    first = jnp.where(lax.axis_index("sp") == 0, REACH, 0).astype(jnp.int32)[None]

    def rows(count):
        return pl.BlockSpec((count, head), lambda h: (0, h))

    line = pl.BlockSpec((1, 1, TABLE), lambda h: (h, 0, 0))

    def shape(count, kind):
        return jax.ShapeDtypeStruct((count, width), kind)

    body = length - REACH
    elements = heads * length * WINDOW
    outs = pl.pallas_call(
        functools.partial(attention_kernel, factor),
        grid=(heads,),
        in_specs=[
            pl.BlockSpec(memory_space=pltpu.SMEM),
            rows(length),
            rows(length),
            rows(length),
            rows(REACH),
            rows(REACH),
            rows(length),
            line,
        ],
        out_specs=[
            rows(length),
            rows(body),
            rows(body),
            rows(REACH),
            rows(REACH),
            rows(REACH),
            rows(REACH),
            line,
        ],
        out_shape=[
            shape(length, jnp.bfloat16),
            shape(body, jnp.bfloat16),
            shape(body, jnp.bfloat16),
            shape(REACH, jnp.float32),
            shape(REACH, jnp.float32),
            shape(REACH, jnp.bfloat16),
            shape(REACH, jnp.bfloat16),
            jax.ShapeDtypeStruct((heads, 1, TABLE), jnp.float32),
        ],
        scratch_shapes=[
            pltpu.VMEM((length + REACH, head), jnp.bfloat16),
            pltpu.VMEM((length + REACH, head), jnp.bfloat16),
            pltpu.VMEM((length + REACH, head), jnp.float32),
            pltpu.VMEM((length + REACH, head), jnp.float32),
        ],
        cost_estimate=pl.CostEstimate(
            flops=10 * elements * head, bytes_accessed=14 * length * width, transcendentals=elements
        ),
    )(first, query, keys, values, prev_keys, prev_values, out_grad, table)
    return outs


def table_to_bias(summed, entries):
    near = summed[:, 1:entries][:, ::-1]
    far = summed[:, :1] + jnp.sum(summed[:, WINDOW:], axis=1, keepdims=True)
    return jnp.concatenate([near, far], axis=1)


def shards(tokens, query_weight, key_weight, value_weight, position_bias, out_grad):
    whole = lax.all_gather(tokens, "tp", axis=1, tiled=True)
    keys = jnp.dot(whole, key_weight, preferred_element_type=jnp.float32).astype(jnp.bfloat16)
    values = jnp.dot(whole, value_weight, preferred_element_type=jnp.float32).astype(jnp.bfloat16)
    length = keys.shape[0]
    prev_keys, prev_values = from_behind(
        (keys[length - REACH :], values[length - REACH :]), "sp", 1
    )
    query = jnp.dot(whole, query_weight, preferred_element_type=jnp.float32).astype(jnp.bfloat16)
    query_grad, key_body, value_body, key_tail, value_tail, key_back, value_back, lines = attention(
        query, keys, values, prev_keys, prev_values, out_grad, position_bias
    )
    key_next, value_next = from_behind((key_back, value_back), "sp", -1)

    def scatter(grad):
        part = contract_rows(whole, grad).astype(jnp.bfloat16)
        return lax.psum_scatter(part, "sp", scatter_dimension=0, tiled=True).astype(jnp.float32)

    query_weight_grad = scatter(query_grad)
    value_grad = jnp.concatenate([value_body, (value_tail + value_next).astype(jnp.bfloat16)])
    value_weight_grad = scatter(value_grad)
    key_grad = jnp.concatenate([key_body, (key_tail + key_next).astype(jnp.bfloat16)])
    key_weight_grad = scatter(key_grad)
    input_part = (
        contract_cols(query_grad, query_weight)
        + contract_cols(key_grad, key_weight)
        + contract_cols(value_grad, value_weight)
    )
    input_grad = lax.psum_scatter(
        input_part.astype(jnp.bfloat16), "tp", scatter_dimension=1, tiled=True
    )
    bias_grad = table_to_bias(lax.psum(lines[:, 0], "sp"), position_bias.shape[1])
    return input_grad, query_weight_grad, key_weight_grad, value_weight_grad, bias_grad


def solution(mesh):
    in_specs = (
        P("sp", "tp"),
        P(None, "tp"),
        P(None, "tp"),
        P(None, "tp"),
        P("tp", None),
        P("sp", "tp"),
    )
    out_specs = (P("sp", "tp"), P("sp", "tp"), P("sp", "tp"), P("sp", "tp"), P("tp", None))
    return jax.shard_map(shards, mesh=mesh, in_specs=in_specs, out_specs=out_specs, check_vma=False)
```

```python
import functools

import jax
import jax.numpy as jnp
from jax import lax
from jax.experimental import pallas as pl
from jax.experimental.pallas import tpu as pltpu
from jax.sharding import PartitionSpec as P

SEGMENT = 64
PREVIOUS = 4
CLIP = 256
ROWS = 2 * SEGMENT
REACH = PREVIOUS * SEGMENT
WINDOW = ROWS + REACH
TABLE = 512
HIDDEN = -1e30


def from_behind(value, axis, steps):
    count = lax.axis_size(axis)
    leading, last = (max(0, -steps), min(count, count - steps))
    return lax.ppermute(value, axis, [(source, source + steps) for source in range(leading, last)])


def contract_rows(left, right):
    return lax.dot_general(
        left, right, (((0,), (0,)), ((), ())), preferred_element_type=jnp.float32
    )


def contract_cols(left, right):
    return lax.dot_general(
        left, right, (((1,), (1,)), ((), ())), preferred_element_type=jnp.float32
    )


def diagonal_sums(tile):
    half = tile.shape[0] // 2
    while half >= 8:
        tile = tile[:half] + pltpu.roll(tile[half:], TABLE - half, 1)
        half //= 2
    row = lax.broadcasted_iota(jnp.int32, tile.shape, 0)
    for step in (4, 2, 1):
        tile = jnp.where((row & step) != 0, pltpu.roll(tile, TABLE - step, 1), tile)
    return jnp.sum(tile, axis=0, keepdims=True)


def attention_kernel(
    factor,
    first_ref,
    q_ref,
    k_ref,
    v_ref,
    pk_ref,
    pv_ref,
    g_ref,
    table_ref,
    dq_ref,
    dk_ref,
    dv_ref,
    dk_tail_ref,
    dv_tail_ref,
    back_ref,
    table_grad_ref,
    k_all,
    v_all,
    dk_all,
    dv_all,
):
    length = q_ref.shape[0]
    k_all[:REACH] = pk_ref[...]
    k_all[REACH:] = k_ref[...]
    v_all[:REACH] = pv_ref[...]
    v_all[REACH:] = v_ref[...]
    dk_all[...] = jnp.zeros_like(dk_all)
    dv_all[...] = jnp.zeros_like(dv_all)
    first = first_ref[0]
    table = jnp.broadcast_to(table_ref[0], (ROWS, TABLE))
    bias = pltpu.roll(table, 0, 1, stride=1, stride_axis=0)[:, :WINDOW]
    row = lax.broadcasted_iota(jnp.int32, (ROWS, WINDOW), 0) // SEGMENT
    column = lax.broadcasted_iota(jnp.int32, (ROWS, WINDOW), 1)
    behind = column // SEGMENT - row
    bias = jnp.where((behind >= 0) & (behind <= PREVIOUS), bias, HIDDEN)
    bias_sum = jnp.zeros((ROWS, WINDOW), jnp.float32)
    for start in range(0, length, ROWS):
        q = q_ref[start : start + ROWS]
        g = g_ref[start : start + ROWS]
        k = k_all[start : start + WINDOW]
        v = v_all[start : start + WINDOW]
        mask = bias
        if start < REACH:
            mask = jnp.where(column + start < first, HIDDEN, bias)
        scores = contract_cols(q, k) * factor + mask
        top = jnp.max(scores, axis=1, keepdims=True)
        raised = jnp.exp(scores - top)
        weights = raised * (1.0 / jnp.sum(raised, axis=1, keepdims=True))
        prob_grad = contract_cols(g, v)
        delta = jnp.sum(weights * prob_grad, axis=1, keepdims=True)
        score_grad = weights * (prob_grad - delta)
        bias_sum = bias_sum + score_grad
        low = score_grad.astype(jnp.bfloat16)
        dq = jnp.dot(low, k, preferred_element_type=jnp.float32) * factor
        dq_ref[start : start + ROWS] = dq.astype(jnp.bfloat16)
        dk_all[start : start + WINDOW] += contract_rows(low, q)
        dv_all[start : start + WINDOW] += contract_rows(weights.astype(jnp.bfloat16), g)
    back_ref[0] = (dk_all[:REACH] * factor).astype(jnp.bfloat16)
    back_ref[1] = dv_all[:REACH].astype(jnp.bfloat16)
    dk_ref[...] = (dk_all[REACH:length] * factor).astype(jnp.bfloat16)
    dv_ref[...] = dv_all[REACH:length].astype(jnp.bfloat16)
    dk_tail_ref[...] = dk_all[length:] * factor
    dv_tail_ref[...] = dv_all[length:]
    padded = jnp.concatenate([bias_sum, jnp.zeros((ROWS, TABLE - WINDOW), jnp.float32)], axis=1)
    table_grad_ref[0] = diagonal_sums(padded)


def attention(query, keys, values, prev_keys, prev_values, out_grad, position_bias):
    length, width = query.shape
    heads, entries = position_bias.shape
    head = width // heads
    factor = head ** (-0.5)
    table = jnp.concatenate(
        [
            position_bias[:, ::-1],
            jnp.zeros((heads, WINDOW - entries), jnp.float32),
            jnp.broadcast_to(position_bias[:, entries - 1 :], (heads, TABLE - WINDOW)),
        ],
        axis=1,
    )[:, None]
    first = jnp.where(lax.axis_index("sp") == 0, REACH, 0).astype(jnp.int32)[None]

    def rows(count):
        return pl.BlockSpec((count, head), lambda h: (0, h))

    line = pl.BlockSpec((1, 1, TABLE), lambda h: (h, 0, 0))

    def shape(count, kind):
        return jax.ShapeDtypeStruct((count, width), kind)

    body = length - REACH
    elements = heads * length * WINDOW
    outs = pl.pallas_call(
        functools.partial(attention_kernel, factor),
        grid=(heads,),
        in_specs=[
            pl.BlockSpec(memory_space=pltpu.SMEM),
            rows(length),
            rows(length),
            rows(length),
            rows(REACH),
            rows(REACH),
            rows(length),
            line,
        ],
        out_specs=[
            rows(length),
            rows(body),
            rows(body),
            rows(REACH),
            rows(REACH),
            pl.BlockSpec((2, REACH, head), lambda h: (0, 0, h)),
            line,
        ],
        out_shape=[
            shape(length, jnp.bfloat16),
            shape(body, jnp.bfloat16),
            shape(body, jnp.bfloat16),
            shape(REACH, jnp.float32),
            shape(REACH, jnp.float32),
            jax.ShapeDtypeStruct((2, REACH, width), jnp.bfloat16),
            jax.ShapeDtypeStruct((heads, 1, TABLE), jnp.float32),
        ],
        scratch_shapes=[
            pltpu.VMEM((length + REACH, head), jnp.bfloat16),
            pltpu.VMEM((length + REACH, head), jnp.bfloat16),
            pltpu.VMEM((length + REACH, head), jnp.float32),
            pltpu.VMEM((length + REACH, head), jnp.float32),
        ],
        cost_estimate=pl.CostEstimate(
            flops=10 * elements * head, bytes_accessed=14 * length * width, transcendentals=elements
        ),
    )(first, query, keys, values, prev_keys, prev_values, out_grad, table)
    return outs


def table_to_bias(summed, entries):
    near = summed[:, 1:entries][:, ::-1]
    far = summed[:, :1] + jnp.sum(summed[:, WINDOW:], axis=1, keepdims=True)
    return jnp.concatenate([near, far], axis=1)


def ring_columns(count):
    columns = 1
    while (2 * columns) ** 2 <= count:
        columns *= 2
    return columns


def ring_place(index, count):
    columns = ring_columns(count)
    rows = count // columns
    row, column = index // columns, index % columns
    above = rows - 1 - row
    across = jnp.where(above % 2 == 0, column - 1, columns - 1 - column)
    return jnp.where(column == 0, row, rows + above * (columns - 1) + across)


def ring_index(place, count):
    columns = ring_columns(count)
    rows = count // columns
    later = jnp.maximum(place - rows, 0)
    above, across = later // (columns - 1), later % (columns - 1)
    column = jnp.where(above % 2 == 0, 1 + across, columns - 1 - across)
    return jnp.where(place < rows, place * columns, (rows - 1 - above) * columns + column)


def ring_kernel(
    count,
    whole_ref,
    dq_ref,
    dk_ref,
    dv_ref,
    line_ref,
    oq_ref,
    ok_ref,
    ov_ref,
    line_out_ref,
    sent,
    got,
    lines,
    send_sem,
    recv_sem,
    line_send,
    line_recv,
):
    me = lax.axis_index("sp")
    place = ring_place(me, count)
    barrier = pltpu.get_barrier_semaphore()
    for ahead in range(1, count):
        peer = lax.rem(me + ahead, count)
        pl.semaphore_signal(
            barrier, inc=1, device_id={"sp": peer}, device_id_type=pl.DeviceIdType.MESH
        )
    pl.semaphore_wait(barrier, count - 1)

    grads = (dq_ref, dk_ref, dv_ref)
    outs = (oq_ref, ok_ref, ov_ref)
    half = sent.shape[3]
    onward = (
        ring_index(lax.rem(place + 1, count), count),
        ring_index(lax.rem(place + count - 1, count), count),
    )

    def own(target, side, chain):
        start = pl.multiple_of((2 * ring_index(target, count) + side) * half, half)
        return contract_rows(whole_ref[:, pl.ds(start, half)], grads[chain][...])

    def target_of(step, side):
        if side == 0:
            return lax.rem(place - 1 - step + 2 * count, count)
        return lax.rem(place + 1 + step, count)

    def copy_of(step, side, chain):
        return pltpu.make_async_remote_copy(
            src_ref=sent.at[side, chain, step],
            dst_ref=got.at[side, chain, step],
            send_sem=send_sem.at[side, chain, step],
            recv_sem=recv_sem.at[side, chain, step],
            device_id={"sp": onward[side]},
            device_id_type=pl.DeviceIdType.MESH,
        )

    def line_copy(ahead):
        return pltpu.make_async_remote_copy(
            src_ref=line_ref,
            dst_ref=lines.at[ahead - 1],
            send_sem=line_send.at[ahead - 1],
            recv_sem=line_recv.at[ahead - 1],
            device_id={"sp": lax.rem(me + ahead, count)},
            device_id_type=pl.DeviceIdType.MESH,
        )

    chains = [(chain, side) for chain in range(3) for side in range(2)]
    for chain, side in chains:
        sent[side, chain, 0] = own(target_of(0, side), side, chain).astype(jnp.bfloat16)
        copy_of(0, side, chain).start()
    for ahead in range(1, count):
        line_copy(ahead).start()

    @pl.loop(1, count - 1)
    def _(step):
        for chain, side in chains:
            part = own(target_of(step, side), side, chain)
            copy_of(step - 1, side, chain).wait_recv()
            total = part + got[side, chain, step - 1].astype(jnp.float32)
            sent[side, chain, step] = total.astype(jnp.bfloat16)
            copy_of(step, side, chain).start()

    total = line_ref[...]
    for ahead in range(1, count):
        line_copy(ahead).wait()
        total = total + lines[ahead - 1]
    line_out_ref[...] = total
    for chain, side in chains:
        part = own(place, side, chain)
        copy_of(count - 2, side, chain).wait_recv()
        total = part + got[side, chain, count - 2].astype(jnp.float32)
        outs[chain][side * half : (side + 1) * half] = total

    @pl.loop(0, count - 1)
    def _(step):
        for chain, side in chains:
            copy_of(step, side, chain).wait_send()


def weight_grads(whole, query_grad, key_grad, value_grad, lines):
    count = lax.axis_size("sp")
    features = whole.shape[1]
    width = query_grad.shape[1]
    half = features // count // 2
    vmem = pl.BlockSpec(memory_space=pltpu.VMEM)
    out = jax.ShapeDtypeStruct((2 * half, width), jnp.float32)
    return pl.pallas_call(
        functools.partial(ring_kernel, count),
        in_specs=[vmem] * 5,
        out_specs=[vmem] * 4,
        out_shape=[out, out, out, jax.ShapeDtypeStruct(lines.shape, jnp.float32)],
        scratch_shapes=[
            pltpu.VMEM((2, 3, count - 1, half, width), jnp.bfloat16),
            pltpu.VMEM((2, 3, count - 1, half, width), jnp.bfloat16),
            pltpu.VMEM((count - 1,) + lines.shape, jnp.float32),
            pltpu.SemaphoreType.DMA((2, 3, count - 1)),
            pltpu.SemaphoreType.DMA((2, 3, count - 1)),
            pltpu.SemaphoreType.DMA((count - 1,)),
            pltpu.SemaphoreType.DMA((count - 1,)),
        ],
        compiler_params=pltpu.CompilerParams(
            collective_id=0, has_side_effects=True, vmem_limit_bytes=56 * 1024 * 1024
        ),
        cost_estimate=pl.CostEstimate(
            flops=6 * whole.shape[0] * features * width,
            bytes_accessed=400_000_000,
            transcendentals=0,
        ),
    )(whole, query_grad, key_grad, value_grad, lines)


def shards(tokens, query_weight, key_weight, value_weight, position_bias, out_grad):
    weights = jnp.concatenate([query_weight, key_weight, value_weight], axis=1)
    whole = lax.all_gather(tokens, "tp", axis=1, tiled=True)
    keys = jnp.dot(whole, key_weight, preferred_element_type=jnp.float32).astype(jnp.bfloat16)
    values = jnp.dot(whole, value_weight, preferred_element_type=jnp.float32).astype(jnp.bfloat16)
    length = keys.shape[0]
    prev_keys, prev_values = from_behind(
        (keys[length - REACH :], values[length - REACH :]), "sp", 1
    )
    query = jnp.dot(whole, query_weight, preferred_element_type=jnp.float32).astype(jnp.bfloat16)
    query_grad, key_body, value_body, key_tail, value_tail, back, lines = attention(
        query, keys, values, prev_keys, prev_values, out_grad, position_bias
    )
    after = from_behind(back, "sp", -1)
    key_grad = jnp.concatenate([key_body, (key_tail + after[0]).astype(jnp.bfloat16)])
    value_grad = jnp.concatenate([value_body, (value_tail + after[1]).astype(jnp.bfloat16)])
    grads = jnp.concatenate([query_grad, key_grad, value_grad], axis=1)
    input_part = contract_cols(grads, weights).astype(jnp.bfloat16)
    input_grad = lax.psum_scatter(input_part, "tp", scatter_dimension=1, tiled=True)
    barrier = lax.optimization_barrier((key_grad, input_part))
    query_weight_grad, key_weight_grad, value_weight_grad, lines = weight_grads(
        whole, query_grad, barrier[0], value_grad, lines[:, 0]
    )
    bias_grad = table_to_bias(lines, position_bias.shape[1])
    return input_grad, query_weight_grad, key_weight_grad, value_weight_grad, bias_grad


def solution(mesh):
    in_specs = (
        P("sp", "tp"),
        P(None, "tp"),
        P(None, "tp"),
        P(None, "tp"),
        P("tp", None),
        P("sp", "tp"),
    )
    out_specs = (P("sp", "tp"), P("sp", "tp"), P("sp", "tp"), P("sp", "tp"), P("tp", None))
    return jax.shard_map(shards, mesh=mesh, in_specs=in_specs, out_specs=out_specs, check_vma=False)
```

```python
import functools

import jax
import jax.numpy as jnp
from jax import lax
from jax.experimental import pallas as pl
from jax.experimental.pallas import tpu as pltpu
from jax.sharding import PartitionSpec as P

SEGMENT = 64
PREVIOUS = 4
CLIP = 256
ROWS = 2 * SEGMENT
REACH = PREVIOUS * SEGMENT
WINDOW = ROWS + REACH
TABLE = 512
HIDDEN = -1e30


def from_behind(value, axis, steps):
    count = lax.axis_size(axis)
    leading, last = (max(0, -steps), min(count, count - steps))
    return lax.ppermute(value, axis, [(source, source + steps) for source in range(leading, last)])


def contract_rows(left, right):
    return lax.dot_general(
        left, right, (((0,), (0,)), ((), ())), preferred_element_type=jnp.float32
    )


def contract_cols(left, right):
    return lax.dot_general(
        left, right, (((1,), (1,)), ((), ())), preferred_element_type=jnp.float32
    )


def diagonal_sums(tile):
    half = tile.shape[0] // 2
    while half >= 8:
        tile = tile[:half] + pltpu.roll(tile[half:], TABLE - half, 1)
        half //= 2
    row = lax.broadcasted_iota(jnp.int32, tile.shape, 0)
    for step in (4, 2, 1):
        tile = jnp.where((row & step) != 0, pltpu.roll(tile, TABLE - step, 1), tile)
    return jnp.sum(tile, axis=0, keepdims=True)


def attention_kernel(
    factor,
    first_ref,
    q_ref,
    k_ref,
    v_ref,
    prev_ref,
    g_ref,
    table_ref,
    dq_ref,
    dk_ref,
    dv_ref,
    dk_tail_ref,
    dv_tail_ref,
    back_ref,
    table_grad_ref,
    k_all,
    v_all,
    dk_all,
    dv_all,
):
    length = q_ref.shape[0]
    k_all[:REACH] = prev_ref[0]
    k_all[REACH:] = k_ref[...]
    v_all[:REACH] = prev_ref[1]
    v_all[REACH:] = v_ref[...]
    dk_all[...] = jnp.zeros_like(dk_all)
    dv_all[...] = jnp.zeros_like(dv_all)
    first = first_ref[0]
    table = jnp.broadcast_to(table_ref[0], (ROWS, TABLE))
    bias = pltpu.roll(table, 0, 1, stride=1, stride_axis=0)[:, :WINDOW]
    row = lax.broadcasted_iota(jnp.int32, (ROWS, WINDOW), 0) // SEGMENT
    column = lax.broadcasted_iota(jnp.int32, (ROWS, WINDOW), 1)
    behind = column // SEGMENT - row
    bias = jnp.where((behind >= 0) & (behind <= PREVIOUS), bias, HIDDEN)
    bias_sum = jnp.zeros((ROWS, WINDOW), jnp.float32)
    for start in range(0, length, ROWS):
        q = q_ref[start : start + ROWS]
        g = g_ref[start : start + ROWS]
        k = k_all[start : start + WINDOW]
        v = v_all[start : start + WINDOW]
        mask = bias
        if start < REACH:
            mask = jnp.where(column + start < first, HIDDEN, bias)
        scores = contract_cols(q, k) * factor + mask
        top = jnp.max(scores, axis=1, keepdims=True)
        raised = jnp.exp(scores - top)
        weights = raised * (1.0 / jnp.sum(raised, axis=1, keepdims=True))
        prob_grad = contract_cols(g, v)
        delta = jnp.sum(weights * prob_grad, axis=1, keepdims=True)
        score_grad = weights * (prob_grad - delta)
        bias_sum = bias_sum + score_grad
        low = score_grad.astype(jnp.bfloat16)
        dq = jnp.dot(low, k, preferred_element_type=jnp.float32) * factor
        dq_ref[start : start + ROWS] = dq.astype(jnp.bfloat16)
        dk_all[start : start + WINDOW] += contract_rows(low, q)
        dv_all[start : start + WINDOW] += contract_rows(weights.astype(jnp.bfloat16), g)
    back_ref[0] = (dk_all[:REACH] * factor).astype(jnp.bfloat16)
    back_ref[1] = dv_all[:REACH].astype(jnp.bfloat16)
    dk_ref[...] = (dk_all[REACH:length] * factor).astype(jnp.bfloat16)
    dv_ref[...] = dv_all[REACH:length].astype(jnp.bfloat16)
    dk_tail_ref[...] = dk_all[length:] * factor
    dv_tail_ref[...] = dv_all[length:]
    padded = jnp.concatenate([bias_sum, jnp.zeros((ROWS, TABLE - WINDOW), jnp.float32)], axis=1)
    table_grad_ref[0] = diagonal_sums(padded)


def attention(query, keys, values, prev, out_grad, position_bias):
    length, width = query.shape
    heads, entries = position_bias.shape
    head = width // heads
    factor = head ** (-0.5)
    table = jnp.concatenate(
        [
            position_bias[:, ::-1],
            jnp.zeros((heads, WINDOW - entries), jnp.float32),
            jnp.broadcast_to(position_bias[:, entries - 1 :], (heads, TABLE - WINDOW)),
        ],
        axis=1,
    )[:, None]
    first = jnp.where(lax.axis_index("sp") == 0, REACH, 0).astype(jnp.int32)[None]

    def rows(count):
        return pl.BlockSpec((count, head), lambda h: (0, h))

    line = pl.BlockSpec((1, 1, TABLE), lambda h: (h, 0, 0))

    def shape(count, kind):
        return jax.ShapeDtypeStruct((count, width), kind)

    body = length - REACH
    elements = heads * length * WINDOW
    outs = pl.pallas_call(
        functools.partial(attention_kernel, factor),
        grid=(heads,),
        in_specs=[
            pl.BlockSpec(memory_space=pltpu.SMEM),
            rows(length),
            rows(length),
            rows(length),
            pl.BlockSpec((2, REACH, head), lambda h: (0, 0, h)),
            rows(length),
            line,
        ],
        out_specs=[
            rows(length),
            rows(body),
            rows(body),
            rows(REACH),
            rows(REACH),
            pl.BlockSpec((2, REACH, head), lambda h: (0, 0, h)),
            line,
        ],
        out_shape=[
            shape(length, jnp.bfloat16),
            shape(body, jnp.bfloat16),
            shape(body, jnp.bfloat16),
            shape(REACH, jnp.float32),
            shape(REACH, jnp.float32),
            jax.ShapeDtypeStruct((2, REACH, width), jnp.bfloat16),
            jax.ShapeDtypeStruct((heads, 1, TABLE), jnp.float32),
        ],
        scratch_shapes=[
            pltpu.VMEM((length + REACH, head), jnp.bfloat16),
            pltpu.VMEM((length + REACH, head), jnp.bfloat16),
            pltpu.VMEM((length + REACH, head), jnp.float32),
            pltpu.VMEM((length + REACH, head), jnp.float32),
        ],
        cost_estimate=pl.CostEstimate(
            flops=10 * elements * head, bytes_accessed=14 * length * width, transcendentals=elements
        ),
    )(first, query, keys, values, prev, out_grad, table)
    return outs


def table_to_bias(summed, entries):
    near = summed[:, 1:entries][:, ::-1]
    far = summed[:, :1] + jnp.sum(summed[:, WINDOW:], axis=1, keepdims=True)
    return jnp.concatenate([near, far], axis=1)


def ring_columns(count):
    columns = 1
    while (2 * columns) ** 2 <= count:
        columns *= 2
    return columns


def ring_place(index, count):
    columns = ring_columns(count)
    rows = count // columns
    row, column = index // columns, index % columns
    above = rows - 1 - row
    across = jnp.where(above % 2 == 0, column - 1, columns - 1 - column)
    return jnp.where(column == 0, row, rows + above * (columns - 1) + across)


def ring_index(place, count):
    columns = ring_columns(count)
    rows = count // columns
    later = jnp.maximum(place - rows, 0)
    above, across = later // (columns - 1), later % (columns - 1)
    column = jnp.where(above % 2 == 0, 1 + across, columns - 1 - across)
    return jnp.where(place < rows, place * columns, (rows - 1 - above) * columns + column)


def ring_kernel(
    count,
    whole_ref,
    dq_ref,
    dk_ref,
    dv_ref,
    line_ref,
    oq_ref,
    ok_ref,
    ov_ref,
    line_out_ref,
    sent,
    got,
    lines,
    send_sem,
    recv_sem,
    line_send,
    line_recv,
):
    me = lax.axis_index("sp")
    place = ring_place(me, count)
    barrier = pltpu.get_barrier_semaphore()
    for ahead in range(1, count):
        peer = lax.rem(me + ahead, count)
        pl.semaphore_signal(
            barrier, inc=1, device_id={"sp": peer}, device_id_type=pl.DeviceIdType.MESH
        )
    pl.semaphore_wait(barrier, count - 1)

    grads = (dq_ref, dk_ref, dv_ref)
    outs = (oq_ref, ok_ref, ov_ref)
    half = sent.shape[3]
    onward = (
        ring_index(lax.rem(place + 1, count), count),
        ring_index(lax.rem(place + count - 1, count), count),
    )

    def own(target, side, chain):
        start = pl.multiple_of((2 * ring_index(target, count) + side) * half, half)
        return contract_rows(whole_ref[:, pl.ds(start, half)], grads[chain][...])

    def target_of(step, side):
        if side == 0:
            return lax.rem(place - 1 - step + 2 * count, count)
        return lax.rem(place + 1 + step, count)

    def copy_of(step, side, chain):
        return pltpu.make_async_remote_copy(
            src_ref=sent.at[side, chain, step],
            dst_ref=got.at[side, chain, step],
            send_sem=send_sem.at[side, chain, step],
            recv_sem=recv_sem.at[side, chain, step],
            device_id={"sp": onward[side]},
            device_id_type=pl.DeviceIdType.MESH,
        )

    def line_copy(ahead):
        return pltpu.make_async_remote_copy(
            src_ref=line_ref,
            dst_ref=lines.at[ahead - 1],
            send_sem=line_send.at[ahead - 1],
            recv_sem=line_recv.at[ahead - 1],
            device_id={"sp": lax.rem(me + ahead, count)},
            device_id_type=pl.DeviceIdType.MESH,
        )

    chains = [(chain, side) for chain in range(3) for side in range(2)]
    for chain, side in chains:
        sent[side, chain, 0] = own(target_of(0, side), side, chain).astype(jnp.bfloat16)
        copy_of(0, side, chain).start()
    for ahead in range(1, count):
        line_copy(ahead).start()

    @pl.loop(1, count - 1)
    def _(step):
        for chain, side in chains:
            part = own(target_of(step, side), side, chain)
            copy_of(step - 1, side, chain).wait_recv()
            total = part + got[side, chain, step - 1].astype(jnp.float32)
            sent[side, chain, step] = total.astype(jnp.bfloat16)
            copy_of(step, side, chain).start()

    total = line_ref[...]
    for ahead in range(1, count):
        line_copy(ahead).wait()
        total = total + lines[ahead - 1]
    line_out_ref[...] = total
    for chain, side in chains:
        part = own(place, side, chain)
        copy_of(count - 2, side, chain).wait_recv()
        total = part + got[side, chain, count - 2].astype(jnp.float32)
        outs[chain][side * half : (side + 1) * half] = total

    @pl.loop(0, count - 1)
    def _(step):
        for chain, side in chains:
            copy_of(step, side, chain).wait_send()


def weight_grads(whole, query_grad, key_grad, value_grad, lines):
    count = lax.axis_size("sp")
    features = whole.shape[1]
    width = query_grad.shape[1]
    half = features // count // 2
    vmem = pl.BlockSpec(memory_space=pltpu.VMEM)
    out = jax.ShapeDtypeStruct((2 * half, width), jnp.float32)
    return pl.pallas_call(
        functools.partial(ring_kernel, count),
        in_specs=[vmem] * 5,
        out_specs=[vmem] * 4,
        out_shape=[out, out, out, jax.ShapeDtypeStruct(lines.shape, jnp.float32)],
        scratch_shapes=[
            pltpu.VMEM((2, 3, count - 1, half, width), jnp.bfloat16),
            pltpu.VMEM((2, 3, count - 1, half, width), jnp.bfloat16),
            pltpu.VMEM((count - 1,) + lines.shape, jnp.float32),
            pltpu.SemaphoreType.DMA((2, 3, count - 1)),
            pltpu.SemaphoreType.DMA((2, 3, count - 1)),
            pltpu.SemaphoreType.DMA((count - 1,)),
            pltpu.SemaphoreType.DMA((count - 1,)),
        ],
        compiler_params=pltpu.CompilerParams(
            collective_id=0, has_side_effects=True, vmem_limit_bytes=56 * 1024 * 1024
        ),
        cost_estimate=pl.CostEstimate(
            flops=6 * whole.shape[0] * features * width,
            bytes_accessed=400_000_000,
            transcendentals=0,
        ),
    )(whole, query_grad, key_grad, value_grad, lines)


def gather_kernel(
    parts,
    tokens_ref,
    wq_ref,
    wk_ref,
    wv_ref,
    whole_ref,
    q_ref,
    k_ref,
    v_ref,
    prev_ref,
    held,
    weights,
    total,
    halo,
    halo_got,
    side_send,
    side_recv,
    far_send,
    far_recv,
    relay_send,
    relay_recv,
    halo_send,
    halo_recv,
    load_sem,
    store_sem,
):
    me = lax.axis_index("tp")
    seat = lax.axis_index("sp")
    seats = lax.axis_size("sp")
    partner = me + 1 - 2 * lax.rem(me, 2)
    chunks = held.shape[0]
    block = tokens_ref.shape[1]
    width = q_ref.shape[1]
    pairs = parts // 2
    matrices = (wq_ref, wk_ref, wv_ref)

    def source(device, away):
        return lax.rem(device + parts - 2 * away, parts)

    order = [me, partner]
    for away in range(1, pairs):
        order += [source(me, away), source(partner, away)]

    def load(slot, matrix):
        start = pl.multiple_of(order[slot] * block, block)
        return pltpu.make_async_copy(
            matrices[matrix].at[pl.ds(start, block)],
            weights.at[slot, matrix],
            load_sem.at[slot, matrix],
        )

    for slot in range(parts):
        for matrix in range(3):
            load(slot, matrix).start()

    barrier = pltpu.get_barrier_semaphore()
    for ahead in range(1, parts):
        pl.semaphore_signal(
            barrier,
            inc=1,
            device_id={"tp": lax.rem(me + ahead, parts)},
            device_id_type=pl.DeviceIdType.MESH,
        )
    onward = lax.rem(seat + 1, seats)
    for other in (onward, lax.rem(seat + seats - 1, seats)):
        pl.semaphore_signal(
            barrier, inc=1, device_id={"sp": other}, device_id_type=pl.DeviceIdType.MESH
        )
    pl.semaphore_wait(barrier, parts + 1)

    def rows(chunk):
        return pl.ds(chunk * REACH, REACH)

    def remote(src, dst, send, recv, device):
        return pltpu.make_async_remote_copy(
            src_ref=src,
            dst_ref=dst,
            send_sem=send,
            recv_sem=recv,
            device_id=device,
            device_id_type=pl.DeviceIdType.MESH,
        )

    def far(chunk, away):
        return remote(
            tokens_ref.at[rows(chunk)],
            held.at[chunk, me],
            far_send.at[chunk, away - 1],
            far_recv.at[chunk, away - 1],
            {"tp": lax.rem(me + 2 * away, parts)},
        )

    def side(chunk):
        return remote(
            tokens_ref.at[rows(chunk)],
            held.at[chunk, me],
            side_send.at[chunk],
            side_recv.at[chunk],
            {"tp": partner},
        )

    def relay(chunk, away):
        place = held.at[chunk, source(me, away)]
        return remote(
            place,
            place,
            relay_send.at[chunk, away - 1],
            relay_recv.at[chunk, away - 1],
            {"tp": partner},
        )

    def neighbour():
        return remote(halo, halo_got, halo_send, halo_recv, {"sp": onward})

    def store(chunk, slot):
        start = pl.multiple_of(order[slot] * block, block)
        src = tokens_ref.at[rows(chunk)] if slot == 0 else held.at[chunk, order[slot]]
        return pltpu.make_async_copy(
            src, whole_ref.at[rows(chunk), pl.ds(start, block)], store_sem.at[chunk, slot]
        )

    def add(chunk, slot, value):
        for matrix in range(3):
            term = jnp.dot(value, weights[slot, matrix], preferred_element_type=jnp.float32)
            if slot == 0:
                total[matrix, chunk] = term
            else:
                total[matrix, chunk] += term

    backwards = list(range(chunks))[::-1]
    for chunk in backwards:
        for away in range(1, pairs):
            far(chunk, away).start()
        side(chunk).start()
    for slot in range(2):
        for matrix in range(3):
            load(slot, matrix).wait()
        for chunk in backwards:
            if slot == 1:
                side(chunk).wait_recv()
            store(chunk, slot).start()
            value = tokens_ref[rows(chunk)] if slot == 0 else held[chunk, partner]
            add(chunk, slot, value)
    for slot in range(2, parts):
        for matrix in range(3):
            load(slot, matrix).wait()
    outs = (q_ref, k_ref, v_ref)
    for chunk in backwards:
        for away in range(1, pairs):
            far(chunk, away).wait_recv()
            relay(chunk, away).start()
            store(chunk, 2 * away).start()
            add(chunk, 2 * away, held[chunk, source(me, away)])
        for away in range(1, pairs):
            relay(chunk, away).wait_recv()
            store(chunk, 2 * away + 1).start()
            add(chunk, 2 * away + 1, held[chunk, source(partner, away)])
        for matrix in range(3):
            outs[matrix][rows(chunk)] = total[matrix, chunk].astype(jnp.bfloat16)
        if chunk == chunks - 1:
            halo[0] = total[1, chunk].astype(jnp.bfloat16)
            halo[1] = total[2, chunk].astype(jnp.bfloat16)
            neighbour().start()
    neighbour().wait()
    prev_ref[...] = halo_got[...]
    for chunk in backwards:
        side(chunk).wait_send()
        for away in range(1, pairs):
            far(chunk, away).wait_send()
            relay(chunk, away).wait_send()
        for slot in range(parts):
            store(chunk, slot).wait()


def project(tokens, query_weight, key_weight, value_weight):
    parts = lax.axis_size("tp")
    length, block = tokens.shape
    width = query_weight.shape[1]
    chunks = length // REACH
    pairs = parts // 2
    vmem = pl.BlockSpec(memory_space=pltpu.VMEM)
    anywhere = pl.BlockSpec(memory_space=pl.ANY)
    narrow = jax.ShapeDtypeStruct((length, width), jnp.bfloat16)
    dma = pltpu.SemaphoreType.DMA
    return pl.pallas_call(
        functools.partial(gather_kernel, parts),
        in_specs=[vmem, anywhere, anywhere, anywhere],
        out_specs=[anywhere, vmem, vmem, vmem, vmem],
        out_shape=[
            jax.ShapeDtypeStruct((length, block * parts), jnp.bfloat16),
            narrow,
            narrow,
            narrow,
            jax.ShapeDtypeStruct((2, REACH, width), jnp.bfloat16),
        ],
        scratch_shapes=[
            pltpu.VMEM((chunks, parts, REACH, block), jnp.bfloat16),
            pltpu.VMEM((parts, 3, block, width), jnp.bfloat16),
            pltpu.VMEM((3, chunks, REACH, width), jnp.float32),
            pltpu.VMEM((2, REACH, width), jnp.bfloat16),
            pltpu.VMEM((2, REACH, width), jnp.bfloat16),
            dma((chunks,)),
            dma((chunks,)),
            dma((chunks, pairs - 1)),
            dma((chunks, pairs - 1)),
            dma((chunks, pairs - 1)),
            dma((chunks, pairs - 1)),
            dma(()),
            dma(()),
            dma((parts, 3)),
            dma((chunks, parts)),
        ],
        compiler_params=pltpu.CompilerParams(
            collective_id=1, has_side_effects=True, vmem_limit_bytes=56 * 1024 * 1024
        ),
        cost_estimate=pl.CostEstimate(
            flops=6 * length * block * parts * width, bytes_accessed=150_000_000, transcendentals=0
        ),
    )(tokens, query_weight, key_weight, value_weight)


def shards(tokens, query_weight, key_weight, value_weight, position_bias, out_grad):
    weights = jnp.concatenate([query_weight, key_weight, value_weight], axis=1)
    whole, query, keys, values, prev = project(tokens, query_weight, key_weight, value_weight)
    query_grad, key_body, value_body, key_tail, value_tail, back, lines = attention(
        query, keys, values, prev, out_grad, position_bias
    )
    after = from_behind(back, "sp", -1)
    key_grad = jnp.concatenate([key_body, (key_tail + after[0]).astype(jnp.bfloat16)])
    value_grad = jnp.concatenate([value_body, (value_tail + after[1]).astype(jnp.bfloat16)])
    grads = jnp.concatenate([query_grad, key_grad, value_grad], axis=1)
    input_part = contract_cols(grads, weights).astype(jnp.bfloat16)
    input_grad = lax.psum_scatter(input_part, "tp", scatter_dimension=1, tiled=True)
    barrier = lax.optimization_barrier((key_grad, input_part))
    query_weight_grad, key_weight_grad, value_weight_grad, lines = weight_grads(
        whole, query_grad, barrier[0], value_grad, lines[:, 0]
    )
    bias_grad = table_to_bias(lines, position_bias.shape[1])
    return input_grad, query_weight_grad, key_weight_grad, value_weight_grad, bias_grad


def solution(mesh):
    in_specs = (
        P("sp", "tp"),
        P(None, "tp"),
        P(None, "tp"),
        P(None, "tp"),
        P("tp", None),
        P("sp", "tp"),
    )
    out_specs = (P("sp", "tp"), P("sp", "tp"), P("sp", "tp"), P("sp", "tp"), P("tp", None))
    return jax.shard_map(shards, mesh=mesh, in_specs=in_specs, out_specs=out_specs, check_vma=False)
```

```python
import functools

import jax
import jax.numpy as jnp
from jax import lax
from jax.experimental import pallas as pl
from jax.experimental.pallas import tpu as pltpu
from jax.sharding import PartitionSpec as P

SEGMENT = 64
PREVIOUS = 4
CLIP = 256
ROWS = 2 * SEGMENT
REACH = PREVIOUS * SEGMENT
WINDOW = ROWS + REACH
TABLE = 512
HIDDEN = -1e30


def from_behind(value, axis, steps):
    count = lax.axis_size(axis)
    leading, last = (max(0, -steps), min(count, count - steps))
    return lax.ppermute(value, axis, [(source, source + steps) for source in range(leading, last)])


def contract_rows(left, right):
    return lax.dot_general(
        left, right, (((0,), (0,)), ((), ())), preferred_element_type=jnp.float32
    )


def contract_cols(left, right):
    return lax.dot_general(
        left, right, (((1,), (1,)), ((), ())), preferred_element_type=jnp.float32
    )


def diagonal_sums(tile):
    half = tile.shape[0] // 2
    while half >= 8:
        tile = tile[:half] + pltpu.roll(tile[half:], TABLE - half, 1)
        half //= 2
    row = lax.broadcasted_iota(jnp.int32, tile.shape, 0)
    for step in (4, 2, 1):
        tile = jnp.where((row & step) != 0, pltpu.roll(tile, TABLE - step, 1), tile)
    return jnp.sum(tile, axis=0, keepdims=True)


def attention_kernel(
    factor,
    first_ref,
    q_ref,
    k_ref,
    v_ref,
    prev_ref,
    g_ref,
    table_ref,
    dq_ref,
    dk_ref,
    dv_ref,
    dk_tail_ref,
    dv_tail_ref,
    back_ref,
    table_grad_ref,
    k_all,
    v_all,
    dk_all,
    dv_all,
):
    length = q_ref.shape[0]
    k_all[:REACH] = prev_ref[0]
    k_all[REACH:] = k_ref[...]
    v_all[:REACH] = prev_ref[1]
    v_all[REACH:] = v_ref[...]
    dk_all[...] = jnp.zeros_like(dk_all)
    dv_all[...] = jnp.zeros_like(dv_all)
    first = first_ref[0]
    table = jnp.broadcast_to(table_ref[0], (ROWS, TABLE))
    bias = pltpu.roll(table, 0, 1, stride=1, stride_axis=0)[:, :WINDOW]
    row = lax.broadcasted_iota(jnp.int32, (ROWS, WINDOW), 0) // SEGMENT
    column = lax.broadcasted_iota(jnp.int32, (ROWS, WINDOW), 1)
    behind = column // SEGMENT - row
    bias = jnp.where((behind >= 0) & (behind <= PREVIOUS), bias, HIDDEN)
    bias_sum = jnp.zeros((ROWS, WINDOW), jnp.float32)
    for start in range(0, length, ROWS):
        q = q_ref[start : start + ROWS]
        g = g_ref[start : start + ROWS]
        k = k_all[start : start + WINDOW]
        v = v_all[start : start + WINDOW]
        mask = bias
        if start < REACH:
            mask = jnp.where(column + start < first, HIDDEN, bias)
        scores = contract_cols(q, k) * factor + mask
        top = jnp.max(scores, axis=1, keepdims=True)
        raised = jnp.exp(scores - top)
        weights = raised * (1.0 / jnp.sum(raised, axis=1, keepdims=True))
        prob_grad = contract_cols(g, v)
        delta = jnp.sum(weights * prob_grad, axis=1, keepdims=True)
        score_grad = weights * (prob_grad - delta)
        bias_sum = bias_sum + score_grad
        low = score_grad.astype(jnp.bfloat16)
        dq = jnp.dot(low, k, preferred_element_type=jnp.float32) * factor
        dq_ref[start : start + ROWS] = dq.astype(jnp.bfloat16)
        dk_all[start : start + WINDOW] += contract_rows(low, q)
        dv_all[start : start + WINDOW] += contract_rows(weights.astype(jnp.bfloat16), g)
    back_ref[0] = (dk_all[:REACH] * factor).astype(jnp.bfloat16)
    back_ref[1] = dv_all[:REACH].astype(jnp.bfloat16)
    dk_ref[...] = (dk_all[REACH:length] * factor).astype(jnp.bfloat16)
    dv_ref[...] = dv_all[REACH:length].astype(jnp.bfloat16)
    dk_tail_ref[...] = dk_all[length:] * factor
    dv_tail_ref[...] = dv_all[length:]
    padded = jnp.concatenate([bias_sum, jnp.zeros((ROWS, TABLE - WINDOW), jnp.float32)], axis=1)
    table_grad_ref[0] = diagonal_sums(padded)


def attention(query, keys, values, prev, out_grad, position_bias):
    length, width = query.shape
    heads, entries = position_bias.shape
    head = width // heads
    factor = head ** (-0.5)
    table = jnp.concatenate(
        [
            position_bias[:, ::-1],
            jnp.zeros((heads, WINDOW - entries), jnp.float32),
            jnp.broadcast_to(position_bias[:, entries - 1 :], (heads, TABLE - WINDOW)),
        ],
        axis=1,
    )[:, None]
    first = jnp.where(lax.axis_index("sp") == 0, REACH, 0).astype(jnp.int32)[None]

    def rows(count):
        return pl.BlockSpec((count, head), lambda h: (0, h))

    line = pl.BlockSpec((1, 1, TABLE), lambda h: (h, 0, 0))

    def shape(count, kind):
        return jax.ShapeDtypeStruct((count, width), kind)

    body = length - REACH
    elements = heads * length * WINDOW
    outs = pl.pallas_call(
        functools.partial(attention_kernel, factor),
        grid=(heads,),
        in_specs=[
            pl.BlockSpec(memory_space=pltpu.SMEM),
            rows(length),
            rows(length),
            rows(length),
            pl.BlockSpec((2, REACH, head), lambda h: (0, 0, h)),
            rows(length),
            line,
        ],
        out_specs=[
            rows(length),
            rows(body),
            rows(body),
            rows(REACH),
            rows(REACH),
            pl.BlockSpec((2, REACH, head), lambda h: (0, 0, h)),
            line,
        ],
        out_shape=[
            shape(length, jnp.bfloat16),
            shape(body, jnp.bfloat16),
            shape(body, jnp.bfloat16),
            shape(REACH, jnp.float32),
            shape(REACH, jnp.float32),
            jax.ShapeDtypeStruct((2, REACH, width), jnp.bfloat16),
            jax.ShapeDtypeStruct((heads, 1, TABLE), jnp.float32),
        ],
        scratch_shapes=[
            pltpu.VMEM((length + REACH, head), jnp.bfloat16),
            pltpu.VMEM((length + REACH, head), jnp.bfloat16),
            pltpu.VMEM((length + REACH, head), jnp.float32),
            pltpu.VMEM((length + REACH, head), jnp.float32),
        ],
        cost_estimate=pl.CostEstimate(
            flops=10 * elements * head, bytes_accessed=14 * length * width, transcendentals=elements
        ),
    )(first, query, keys, values, prev, out_grad, table)
    return outs


def table_to_bias(summed, entries):
    near = summed[:, 1:entries][:, ::-1]
    far = summed[:, :1] + jnp.sum(summed[:, WINDOW:], axis=1, keepdims=True)
    return jnp.concatenate([near, far], axis=1)


def ring_columns(count):
    columns = 1
    while (2 * columns) ** 2 <= count:
        columns *= 2
    return columns


def ring_place(index, count):
    columns = ring_columns(count)
    rows = count // columns
    row, column = index // columns, index % columns
    above = rows - 1 - row
    across = jnp.where(above % 2 == 0, column - 1, columns - 1 - column)
    return jnp.where(column == 0, row, rows + above * (columns - 1) + across)


def ring_index(place, count):
    columns = ring_columns(count)
    rows = count // columns
    later = jnp.maximum(place - rows, 0)
    above, across = later // (columns - 1), later % (columns - 1)
    column = jnp.where(above % 2 == 0, 1 + across, columns - 1 - across)
    return jnp.where(place < rows, place * columns, (rows - 1 - above) * columns + column)


def ring_kernel(
    count,
    whole_ref,
    dq_ref,
    dk_ref,
    dv_ref,
    line_ref,
    oq_ref,
    ok_ref,
    ov_ref,
    line_out_ref,
    sent,
    got,
    lines,
    send_sem,
    recv_sem,
    line_send,
    line_recv,
):
    me = lax.axis_index("sp")
    place = ring_place(me, count)
    barrier = pltpu.get_barrier_semaphore()
    for ahead in range(1, count):
        peer = lax.rem(me + ahead, count)
        pl.semaphore_signal(
            barrier, inc=1, device_id={"sp": peer}, device_id_type=pl.DeviceIdType.MESH
        )
    pl.semaphore_wait(barrier, count - 1)

    grads = (dq_ref, dk_ref, dv_ref)
    outs = (oq_ref, ok_ref, ov_ref)
    half = sent.shape[3]
    onward = (
        ring_index(lax.rem(place + 1, count), count),
        ring_index(lax.rem(place + count - 1, count), count),
    )

    def own(target, side, chain):
        start = pl.multiple_of((2 * ring_index(target, count) + side) * half, half)
        return contract_rows(whole_ref[:, pl.ds(start, half)], grads[chain][...])

    def target_of(step, side):
        if side == 0:
            return lax.rem(place - 1 - step + 2 * count, count)
        return lax.rem(place + 1 + step, count)

    def copy_of(step, side, chain):
        return pltpu.make_async_remote_copy(
            src_ref=sent.at[side, chain, step],
            dst_ref=got.at[side, chain, step],
            send_sem=send_sem.at[side, chain, step],
            recv_sem=recv_sem.at[side, chain, step],
            device_id={"sp": onward[side]},
            device_id_type=pl.DeviceIdType.MESH,
        )

    def line_copy(ahead):
        return pltpu.make_async_remote_copy(
            src_ref=line_ref,
            dst_ref=lines.at[ahead - 1],
            send_sem=line_send.at[ahead - 1],
            recv_sem=line_recv.at[ahead - 1],
            device_id={"sp": lax.rem(me + ahead, count)},
            device_id_type=pl.DeviceIdType.MESH,
        )

    chains = [(chain, side) for chain in range(3) for side in range(2)]
    for chain, side in chains:
        sent[side, chain, 0] = own(target_of(0, side), side, chain).astype(jnp.bfloat16)
        copy_of(0, side, chain).start()
    for ahead in range(1, count):
        line_copy(ahead).start()

    @pl.loop(1, count - 1)
    def _(step):
        for chain, side in chains:
            part = own(target_of(step, side), side, chain)
            copy_of(step - 1, side, chain).wait_recv()
            total = part + got[side, chain, step - 1].astype(jnp.float32)
            sent[side, chain, step] = total.astype(jnp.bfloat16)
            copy_of(step, side, chain).start()

    total = line_ref[...]
    for ahead in range(1, count):
        line_copy(ahead).wait()
        total = total + lines[ahead - 1]
    line_out_ref[...] = total
    for chain, side in chains:
        part = own(place, side, chain)
        copy_of(count - 2, side, chain).wait_recv()
        total = part + got[side, chain, count - 2].astype(jnp.float32)
        outs[chain][side * half : (side + 1) * half] = total

    @pl.loop(0, count - 1)
    def _(step):
        for chain, side in chains:
            copy_of(step, side, chain).wait_send()


def weight_grads(whole, query_grad, key_grad, value_grad, lines):
    count = lax.axis_size("sp")
    features = whole.shape[1]
    width = query_grad.shape[1]
    half = features // count // 2
    vmem = pl.BlockSpec(memory_space=pltpu.VMEM)
    out = jax.ShapeDtypeStruct((2 * half, width), jnp.float32)
    return pl.pallas_call(
        functools.partial(ring_kernel, count),
        in_specs=[vmem] * 5,
        out_specs=[vmem] * 4,
        out_shape=[out, out, out, jax.ShapeDtypeStruct(lines.shape, jnp.float32)],
        scratch_shapes=[
            pltpu.VMEM((2, 3, count - 1, half, width), jnp.bfloat16),
            pltpu.VMEM((2, 3, count - 1, half, width), jnp.bfloat16),
            pltpu.VMEM((count - 1,) + lines.shape, jnp.float32),
            pltpu.SemaphoreType.DMA((2, 3, count - 1)),
            pltpu.SemaphoreType.DMA((2, 3, count - 1)),
            pltpu.SemaphoreType.DMA((count - 1,)),
            pltpu.SemaphoreType.DMA((count - 1,)),
        ],
        compiler_params=pltpu.CompilerParams(
            collective_id=0, has_side_effects=True, vmem_limit_bytes=56 * 1024 * 1024
        ),
        cost_estimate=pl.CostEstimate(
            flops=6 * whole.shape[0] * features * width,
            bytes_accessed=400_000_000,
            transcendentals=0,
        ),
    )(whole, query_grad, key_grad, value_grad, lines)


def gather_kernel(
    parts,
    tokens_ref,
    wq_ref,
    wk_ref,
    wv_ref,
    whole_ref,
    q_ref,
    k_ref,
    v_ref,
    prev_ref,
    held,
    weights,
    total,
    halo,
    halo_got,
    side_send,
    side_recv,
    far_send,
    far_recv,
    relay_send,
    relay_recv,
    halo_send,
    halo_recv,
    load_sem,
    store_sem,
):
    me = lax.axis_index("tp")
    seat = lax.axis_index("sp")
    seats = lax.axis_size("sp")
    partner = me + 1 - 2 * lax.rem(me, 2)
    chunks = held.shape[0]
    block = tokens_ref.shape[1]
    width = q_ref.shape[1]
    pairs = parts // 2
    matrices = (wq_ref, wk_ref, wv_ref)

    def source(device, away):
        return lax.rem(device + parts - 2 * away, parts)

    order = [me, partner]
    for away in range(1, pairs):
        order += [source(me, away), source(partner, away)]

    def load(slot, matrix):
        start = pl.multiple_of(order[slot] * block, block)
        return pltpu.make_async_copy(
            matrices[matrix].at[pl.ds(start, block)],
            weights.at[slot, matrix],
            load_sem.at[slot, matrix],
        )

    for slot in range(parts):
        for matrix in range(3):
            load(slot, matrix).start()

    barrier = pltpu.get_barrier_semaphore()
    for ahead in range(1, parts):
        pl.semaphore_signal(
            barrier,
            inc=1,
            device_id={"tp": lax.rem(me + ahead, parts)},
            device_id_type=pl.DeviceIdType.MESH,
        )
    onward = lax.rem(seat + 1, seats)
    for other in (onward, lax.rem(seat + seats - 1, seats)):
        pl.semaphore_signal(
            barrier, inc=1, device_id={"sp": other}, device_id_type=pl.DeviceIdType.MESH
        )
    pl.semaphore_wait(barrier, parts + 1)

    def rows(chunk):
        return pl.ds(chunk * REACH, REACH)

    def remote(src, dst, send, recv, device):
        return pltpu.make_async_remote_copy(
            src_ref=src,
            dst_ref=dst,
            send_sem=send,
            recv_sem=recv,
            device_id=device,
            device_id_type=pl.DeviceIdType.MESH,
        )

    def far(chunk, away):
        return remote(
            tokens_ref.at[rows(chunk)],
            held.at[chunk, me],
            far_send.at[chunk, away - 1],
            far_recv.at[chunk, away - 1],
            {"tp": lax.rem(me + 2 * away, parts)},
        )

    def side(chunk):
        return remote(
            tokens_ref.at[rows(chunk)],
            held.at[chunk, me],
            side_send.at[chunk],
            side_recv.at[chunk],
            {"tp": partner},
        )

    def relay(chunk, away):
        place = held.at[chunk, source(me, away)]
        return remote(
            place,
            place,
            relay_send.at[chunk, away - 1],
            relay_recv.at[chunk, away - 1],
            {"tp": partner},
        )

    def neighbour():
        return remote(halo, halo_got, halo_send, halo_recv, {"sp": onward})

    def store(chunk, slot):
        start = pl.multiple_of(order[slot] * block, block)
        src = tokens_ref.at[rows(chunk)] if slot == 0 else held.at[chunk, order[slot]]
        return pltpu.make_async_copy(
            src, whole_ref.at[rows(chunk), pl.ds(start, block)], store_sem.at[chunk, slot]
        )

    def add(chunk, slot, value):
        for matrix in range(3):
            term = jnp.dot(value, weights[slot, matrix], preferred_element_type=jnp.float32)
            if slot == 0:
                total[matrix, chunk] = term
            else:
                total[matrix, chunk] += term

    backwards = list(range(chunks))[::-1]
    for chunk in backwards:
        for away in range(1, pairs):
            far(chunk, away).start()
        side(chunk).start()
    for slot in range(2):
        for matrix in range(3):
            load(slot, matrix).wait()
        for chunk in backwards:
            if slot == 1:
                side(chunk).wait_recv()
            store(chunk, slot).start()
            value = tokens_ref[rows(chunk)] if slot == 0 else held[chunk, partner]
            add(chunk, slot, value)
    for slot in range(2, parts):
        for matrix in range(3):
            load(slot, matrix).wait()
    outs = (q_ref, k_ref, v_ref)
    for chunk in backwards:
        for away in range(1, pairs):
            far(chunk, away).wait_recv()
            relay(chunk, away).start()
            store(chunk, 2 * away).start()
            add(chunk, 2 * away, held[chunk, source(me, away)])
        for away in range(1, pairs):
            relay(chunk, away).wait_recv()
            store(chunk, 2 * away + 1).start()
            add(chunk, 2 * away + 1, held[chunk, source(partner, away)])
        for matrix in range(3):
            outs[matrix][rows(chunk)] = total[matrix, chunk].astype(jnp.bfloat16)
        if chunk == chunks - 1:
            halo[0] = total[1, chunk].astype(jnp.bfloat16)
            halo[1] = total[2, chunk].astype(jnp.bfloat16)
            neighbour().start()
    neighbour().wait()
    prev_ref[...] = halo_got[...]
    for chunk in backwards:
        side(chunk).wait_send()
        for away in range(1, pairs):
            far(chunk, away).wait_send()
            relay(chunk, away).wait_send()
        for slot in range(parts):
            store(chunk, slot).wait()


def project(tokens, query_weight, key_weight, value_weight):
    parts = lax.axis_size("tp")
    length, block = tokens.shape
    width = query_weight.shape[1]
    chunks = length // REACH
    pairs = parts // 2
    vmem = pl.BlockSpec(memory_space=pltpu.VMEM)
    anywhere = pl.BlockSpec(memory_space=pl.ANY)
    narrow = jax.ShapeDtypeStruct((length, width), jnp.bfloat16)
    dma = pltpu.SemaphoreType.DMA
    return pl.pallas_call(
        functools.partial(gather_kernel, parts),
        in_specs=[vmem, anywhere, anywhere, anywhere],
        out_specs=[anywhere, vmem, vmem, vmem, vmem],
        out_shape=[
            jax.ShapeDtypeStruct((length, block * parts), jnp.bfloat16),
            narrow,
            narrow,
            narrow,
            jax.ShapeDtypeStruct((2, REACH, width), jnp.bfloat16),
        ],
        scratch_shapes=[
            pltpu.VMEM((chunks, parts, REACH, block), jnp.bfloat16),
            pltpu.VMEM((parts, 3, block, width), jnp.bfloat16),
            pltpu.VMEM((3, chunks, REACH, width), jnp.float32),
            pltpu.VMEM((2, REACH, width), jnp.bfloat16),
            pltpu.VMEM((2, REACH, width), jnp.bfloat16),
            dma((chunks,)),
            dma((chunks,)),
            dma((chunks, pairs - 1)),
            dma((chunks, pairs - 1)),
            dma((chunks, pairs - 1)),
            dma((chunks, pairs - 1)),
            dma(()),
            dma(()),
            dma((parts, 3)),
            dma((chunks, parts)),
        ],
        compiler_params=pltpu.CompilerParams(
            collective_id=1, has_side_effects=True, vmem_limit_bytes=56 * 1024 * 1024
        ),
        cost_estimate=pl.CostEstimate(
            flops=6 * length * block * parts * width, bytes_accessed=150_000_000, transcendentals=0
        ),
    )(tokens, query_weight, key_weight, value_weight)


def shards(tokens, query_weight, key_weight, value_weight, position_bias, out_grad):
    weights = jnp.concatenate([query_weight, key_weight, value_weight], axis=1)
    whole, query, keys, values, prev = project(tokens, query_weight, key_weight, value_weight)
    query_grad, key_body, value_body, key_tail, value_tail, back, lines = attention(
        query, keys, values, prev, out_grad, position_bias
    )
    after = from_behind(back, "sp", -1)
    body = key_body.shape[0]
    body_grads = jnp.concatenate([query_grad[:body], key_body, value_body], axis=1)
    body_part = contract_cols(body_grads, weights).astype(jnp.bfloat16)
    after, body_part = lax.optimization_barrier((after, body_part))
    key_last = (key_tail + after[0]).astype(jnp.bfloat16)
    value_last = (value_tail + after[1]).astype(jnp.bfloat16)
    last_grads = jnp.concatenate([query_grad[body:], key_last, value_last], axis=1)
    last_part = contract_cols(last_grads, weights).astype(jnp.bfloat16)
    key_grad = jnp.concatenate([key_body, key_last])
    value_grad = jnp.concatenate([value_body, value_last])
    input_grad = jnp.concatenate(
        [
            lax.psum_scatter(part, "tp", scatter_dimension=1, tiled=True)
            for part in (body_part, last_part)
        ]
    )
    barrier = lax.optimization_barrier((key_grad, body_part, last_part))
    query_weight_grad, key_weight_grad, value_weight_grad, lines = weight_grads(
        whole, query_grad, barrier[0], value_grad, lines[:, 0]
    )
    bias_grad = table_to_bias(lines, position_bias.shape[1])
    return input_grad, query_weight_grad, key_weight_grad, value_weight_grad, bias_grad


def solution(mesh):
    in_specs = (
        P("sp", "tp"),
        P(None, "tp"),
        P(None, "tp"),
        P(None, "tp"),
        P("tp", None),
        P("sp", "tp"),
    )
    out_specs = (P("sp", "tp"), P("sp", "tp"), P("sp", "tp"), P("sp", "tp"), P("tp", None))
    return jax.shard_map(shards, mesh=mesh, in_specs=in_specs, out_specs=out_specs, check_vma=False)
```
